32 devices in a mesh: ep: 8 (over z, y), tp: 4 (over x, core).
Axes of the slice: x: 2, y: 2, z: 4, core: 2. Of those that a mesh axis runs over, the one named last changes fastest.
Arguments:
- tokens: bfloat16 [192, 1024], P('ep'), may hold values from -6 to 6
- mixer_gain: float32 [1024], replicated, may hold values from 0.1 to 1.9
- gate_weight: bfloat16 [1024, 1024], P(None, 'tp'), may hold values from -0.1875 to 0.1875
- inner_weight: bfloat16 [1024, 1024], P(None, 'tp'), may hold values from -0.1875 to 0.1875
- state_weight: bfloat16 [2, 1024, 512], P(None, None, 'tp'), may hold values from -0.1875 to 0.1875
- step_weight: bfloat16 [1024, 16], P(None, 'tp'), may hold values from -0.1875 to 0.1875
- step_bias: float32 [16], P('tp'), may hold values from -4 to 0.5
- decay_log: float32 [16], P('tp'), may hold values from 0 to 2.8
- skip_scale: float32 [16], P('tp'), may hold values from 0.5 to 1.5
- inner_kernel: float32 [4, 1024], P(None, 'tp'), may hold values from -3 to 3
- state_kernel: float32 [4, 2, 512], P(None, None, 'tp'), may hold values from -3 to 3
- inner_window: bfloat16 [192, 3, 1024], P('ep', None, 'tp'), may hold values from -6 to 6
- state_window: bfloat16 [192, 3, 2, 512], P('ep', None, None, 'tp'), may hold values from -6 to 6
- recurrent_state: float32 [192, 16, 64, 128], P('ep', 'tp'), may hold values from -2.4 to 2.4
- group_gain: float32 [1024], P('tp'), may hold values from 0.1 to 1.9
- output_weight: bfloat16 [1024, 1024], P('tp'), may hold values from -0.1875 to 0.1875
- channel_gain: float32 [1024], replicated, may hold values from 0.1 to 1.9
- routes: int32 [192, 2], P('ep'), may hold values from 0 to 7, all different within a row; in each aligned block of 24 rows (0 to 23, 24 to 47, ...) at most 9 rows name the same one
- route_weights: float32 [192, 2], P('ep'), may hold values from 0.2 to 1
- expert_gate: bfloat16 [8, 1024, 2816], P('ep', None, 'tp'), may hold values from -0.1875 to 0.1875
- expert_up: bfloat16 [8, 1024, 2816], P('ep', None, 'tp'), may hold values from -0.1875 to 0.1875
- expert_down: bfloat16 [8, 2816, 1024], P('ep', 'tp'), may hold values from -0.109375 to 0.109375
- dense_gate: bfloat16 [1024, 2816], P('tp', 'ep'), may hold values from -0.1875 to 0.1875
- dense_up: bfloat16 [1024, 2816], P('tp', 'ep'), may hold values from -0.1875 to 0.1875
- dense_down: bfloat16 [2816, 1024], P('ep', 'tp'), may hold values from -0.109375 to 0.109375
- dense_scale: float32 [1024], P('tp'), may hold values from 0.3 to 1.5
Outputs:
- new_tokens: bfloat16 [192, 1024], P('ep', 'tp')
- new_state: float32 [192, 16, 64, 128], P('ep', 'tp')
- new_inner_window: bfloat16 [192, 3, 1024], P('ep', None, 'tp')
- new_state_window: bfloat16 [192, 3, 2, 512], P('ep', None, None, 'tp')
The draws below stay inside these ranges and needn't reach their ends.
Inputs may be any that keep to these rules, and one draw needn't show every extreme that they name: `routes`: each row names 2 different experts. Within the rows of one device (aligned blocks of 24 rows) no expert is named by more than 9 rows, and in some block an expert is named by exactly 9 rows.
All inputs are finite; a program needn't handle non-finite values.
Results may differ from the reference program's by a relative error of at most 0.014.
Values may be sent and summed in bfloat16 or wider, within the bound.
A program may use at most 64 MiB of HBM per device.

```python
import math
import jax
import jax.numpy as jnp
import numpy as np
from jax import lax

D = 1024
HEADS = 16
GROUPS = 4
HEAD_DIM = 64
STATE_DIM = 128
CONV = 4
FF = 2816
FFD = 2816
TOPK = 2
S_DEV = 24
EXPERTS = 8
BATCH = 192
INNER = 1024
BC = 512
CAP = 9
N_EP = 8
N_TP = 4


def steps_of(own_key, dims, pieces, low, high):
    loudness, own = 1.0, jax.random.fold_in(own_key, 6)
    for axis_at, parts in pieces:
        draws = jnp.exp(jax.random.uniform(jax.random.fold_in(own, axis_at), (parts,), jnp.float32, low / len(pieces), high / len(pieces)))
        loudness = loudness * jnp.repeat(draws, dims[axis_at] // parts).reshape([-1 if axis == axis_at else 1 for axis in range(len(dims))])
    return loudness


def deal_out(own_key, own, number, rows, amount, top, bound, slope):
    order = jax.random.permutation(own_key, amount)
    crowded, ordinary = shares(amount, rows * top, bound, slope, True), shares(amount, rows * top, bound, slope, False)
    places = jnp.arange(amount)

    def named(sizes, offset_by):
        used = int((sizes > 0).sum())
        fixed = max(1, used // 4)
        shifted = fixed + (places - fixed + offset_by * (used - fixed)) % max(1, amount - fixed)
        return jnp.zeros((amount,), jnp.int32).at[order[jnp.where(places < fixed, places, shifted)]].set(jnp.asarray(sizes, jnp.int32))

    sizes = jnp.where(number % 4 == 0, named(crowded, number // 4), named(ordinary, number - number // 4 - 1))
    mixed = jax.random.permutation(jax.random.fold_in(own, 3), amount)
    giver, sink = mixed[0:amount // 2 * 2:2], mixed[1:amount // 2 * 2:2]
    room = jnp.minimum(sizes[giver] - 1, bound - sizes[sink]) // 2
    room = jnp.where((giver == order[0]) | (sink == order[0]) | (sizes[sink] == 0), 0, jnp.maximum(room, 0))
    shifted = jax.random.randint(jax.random.fold_in(own, 4), (amount // 2,), 0, 1 << 20) % (room + 1)
    sizes = sizes.at[giver].add(-shifted).at[sink].add(shifted)
    items = jnp.searchsorted(jnp.cumsum(sizes), jnp.arange(rows * top), side="right").astype(jnp.int32)
    listing = items.reshape(top, rows).T
    listing = listing[jax.random.permutation(jax.random.fold_in(own, 1), rows)]
    offset_by = jax.random.randint(jax.random.fold_in(own, 2), (rows, 1), 0, top)
    return jnp.take_along_axis(listing, (jnp.arange(top)[None, :] + offset_by) % top, axis=1)


def shares(count, total, bound, skew, full):
    weights = [(1 << 20) // math.isqrt(rank ** skew) + 1 for rank in range(1, count + 1)]
    largest = bound if full else min(bound, max(-(-total // count), total * weights[0] // sum(weights)))
    least = 1 if total - largest >= count - 1 else 0
    given, spare = [largest] + [least] * (count - 1), total - largest - least * (count - 1)
    while spare > 0:
        candidates = [i for i in range(1, count) if given[i] < largest] or [i for i in range(1, count) if given[i] < bound]
        pool, left = sum([weights[i] for i in candidates]), spare
        for i in candidates:
            addition = min(bound - given[i], max(1, left * weights[i] // pool), spare)
            given[i] = given[i] + addition
            spare = spare - addition
    return np.array(given)


def noise(own_key, extent, spread, most, shards=(), kind=jnp.bfloat16):
    array = jax.random.normal(own_key, extent, jnp.float32) * spread
    if len(shards) > 0:
        array = steps_of(own_key, extent, shards, -0.22, 0.18) * array
    return jnp.clip(array, min=-most, max=most).astype(kind)


def setup_inputs(seed: int = 0) -> dict:
    arg_keys = jax.random.split(jax.random.key(seed), 27)
    tokens = noise(arg_keys[0], (BATCH, D), 1.0, 6.0, ((0, 8),))
    mixer_gain = jnp.clip(1.0 + 0.18 * jax.random.normal(arg_keys[1], (D,), jnp.float32), 0.1, 1.9)
    gate_weight = noise(arg_keys[2], (D, INNER), D ** -0.5, 0.1875, ((1, 4),))
    inner_weight = noise(arg_keys[3], (D, INNER), D ** -0.5, 0.1875, ((1, 4),))
    state_weight = noise(arg_keys[4], (2, D, BC), D ** -0.5, 0.1875, ((2, 4),))
    step_weight = noise(arg_keys[5], (D, HEADS), D ** -0.5, 0.1875, ((1, 4),))
    step_bias = jnp.clip(-4.0 + 4.5 * jax.random.uniform(arg_keys[6], (HEADS,), jnp.float32) ** steps_of(arg_keys[6], (HEADS,), ((0, 4),), -0.2, 0.2), -4.0, 0.5)
    decay_log = jnp.clip(2.8 * jax.random.uniform(arg_keys[7], (HEADS,), jnp.float32) ** steps_of(arg_keys[7], (HEADS,), ((0, 4),), -0.2, 0.2), 0.0, 2.8)
    skip_scale = jnp.clip(0.5 + 1.0 * jax.random.uniform(arg_keys[8], (HEADS,), jnp.float32) ** steps_of(arg_keys[8], (HEADS,), ((0, 4),), -0.2, 0.2), 0.5, 1.5)
    inner_kernel = noise(arg_keys[9], (CONV, INNER), CONV ** -0.5, 3.0, ((1, 4),), jnp.float32)
    state_kernel = noise(arg_keys[10], (CONV, 2, BC), CONV ** -0.5, 3.0, ((2, 4),), jnp.float32)
    inner_window = noise(arg_keys[11], (BATCH, CONV - 1, INNER), 1.0, 6.0, ((0, 8), (2, 4)))
    state_window = noise(arg_keys[12], (BATCH, CONV - 1, 2, BC), 1.0, 6.0, ((0, 8), (3, 4)))
    recurrent_state = noise(arg_keys[13], (BATCH, HEADS, HEAD_DIM, STATE_DIM), 0.3, 2.4, ((0, 8), (1, 4)), jnp.float32)
    group_gain = jnp.clip(1.0 + 0.18 * jax.random.normal(arg_keys[14], (INNER,), jnp.float32), 0.1, 1.9)
    output_weight = noise(arg_keys[15], (INNER, D), INNER ** -0.5, 0.1875, ((0, 4),))
    channel_gain = jnp.clip(1.0 + 0.18 * jax.random.normal(arg_keys[16], (D,), jnp.float32), 0.1, 1.9)
    routes_keys = jax.random.split(jax.random.fold_in(arg_keys[17], 1), BATCH // S_DEV)
    routes_turns = jax.random.permutation(jax.random.fold_in(arg_keys[17], 3), BATCH // S_DEV)
    routes = jax.vmap(lambda own, number: deal_out(jax.random.fold_in(arg_keys[17], 2), own, number, S_DEV, EXPERTS, TOPK, CAP, 2))(routes_keys, routes_turns).reshape((BATCH, TOPK))
    route_weights = jnp.clip(0.2 + 0.8 * jax.random.uniform(arg_keys[18], (BATCH, TOPK), jnp.float32) ** steps_of(arg_keys[18], (BATCH, TOPK), ((0, 8),), -0.2, 0.2), 0.2, 1.0)
    expert_gate = noise(arg_keys[19], (EXPERTS, D, FF), D ** -0.5, 0.1875, ((0, 8), (2, 4)))
    expert_up = noise(arg_keys[20], (EXPERTS, D, FF), D ** -0.5, 0.1875, ((0, 8), (2, 4)))
    expert_down = noise(arg_keys[21], (EXPERTS, FF, D), FF ** -0.5, 0.109375, ((0, 8), (1, 4)))
    dense_gate = noise(arg_keys[22], (D, FFD), D ** -0.5, 0.1875, ((0, 4), (1, 8)))
    dense_up = noise(arg_keys[23], (D, FFD), D ** -0.5, 0.1875, ((0, 4), (1, 8)))
    dense_down = noise(arg_keys[24], (FFD, D), FFD ** -0.5, 0.109375, ((0, 8), (1, 4)))
    dense_scale = jnp.clip(0.3 + 1.2 * jax.random.uniform(arg_keys[25], (D,), jnp.float32) ** steps_of(arg_keys[25], (D,), ((0, 4),), -0.2, 0.2), 0.3, 1.5)
    return {"tokens": tokens, "mixer_gain": mixer_gain, "gate_weight": gate_weight, "inner_weight": inner_weight, "state_weight": state_weight, "step_weight": step_weight, "step_bias": step_bias, "decay_log": decay_log, "skip_scale": skip_scale, "inner_kernel": inner_kernel, "state_kernel": state_kernel, "inner_window": inner_window, "state_window": state_window, "recurrent_state": recurrent_state, "group_gain": group_gain, "output_weight": output_weight, "channel_gain": channel_gain, "routes": routes, "route_weights": route_weights, "expert_gate": expert_gate, "expert_up": expert_up, "expert_down": expert_down, "dense_gate": dense_gate, "dense_up": dense_up, "dense_down": dense_down, "dense_scale": dense_scale}


eps = 1e-06

def rms_scale(values, norm_gain):
    squares = lax.optimization_barrier(jnp.mean(values * values, axis=-1, keepdims=True))
    return values * lax.rsqrt(squares + eps) * norm_gain

def reference(tokens, mixer_gain, gate_weight, inner_weight, state_weight, step_weight, step_bias, decay_log, skip_scale, inner_kernel, state_kernel, inner_window, state_window, recurrent_state, group_gain, output_weight, channel_gain, routes, route_weights, expert_gate, expert_up, expert_down, dense_gate, dense_up, dense_down, dense_scale):
    f32 = jnp.float32
    bf16 = jnp.bfloat16
    residual = tokens.astype(f32)
    normed = rms_scale(residual, mixer_gain).astype(bf16)
    gate_pre = jnp.dot(normed, gate_weight, preferred_element_type=f32)
    inner_pre = jnp.dot(normed, inner_weight, preferred_element_type=f32).astype(bf16)
    state_pre = jnp.stack([jnp.dot(normed, state_weight[0], preferred_element_type=f32), jnp.dot(normed, state_weight[1], preferred_element_type=f32)], axis=1).astype(bf16)
    step_raw = jnp.dot(normed, step_weight, preferred_element_type=f32)
    inner_ctx = jnp.concatenate([inner_window, inner_pre[:, None, :]], axis=1)
    inner_conv = jax.nn.silu(lax.optimization_barrier(jnp.sum(inner_ctx.astype(f32) * inner_kernel[None], axis=1)))
    state_ctx = jnp.concatenate([state_window, state_pre[:, None]], axis=1)
    state_conv = jax.nn.silu(lax.optimization_barrier(jnp.sum(state_ctx.astype(f32) * state_kernel[None], axis=1)))
    per_group = HEADS // GROUPS
    step_size = jax.nn.softplus(step_raw + step_bias)
    decay_rate = jnp.exp(-step_size * jnp.exp(decay_log))
    shaped = (BATCH, GROUPS, per_group)
    inner_heads = inner_conv.reshape(BATCH, GROUPS, per_group, HEAD_DIM)
    in_vector = state_conv[:, 0].reshape(BATCH, GROUPS, STATE_DIM)
    out_vector = state_conv[:, 1].reshape(BATCH, GROUPS, STATE_DIM)
    old_state = recurrent_state.reshape(BATCH, GROUPS, per_group, HEAD_DIM, STATE_DIM)
    written = (step_size.reshape(shaped)[..., None] * inner_heads)[..., None] * in_vector[:, :, None, None, :]
    new_state = old_state * decay_rate.reshape(shaped)[..., None, None] + written
    mixed_out = jnp.einsum('sgrpn,sgn->sgrp', new_state, out_vector, precision=lax.Precision.HIGHEST)
    mixed_out = mixed_out + skip_scale.reshape(GROUPS, per_group)[None, :, :, None] * inner_heads
    gated_out = mixed_out.reshape(BATCH, INNER) * jax.nn.silu(gate_pre)
    grouped = rms_scale(gated_out.reshape(BATCH, GROUPS, -1), 1.0).reshape(BATCH, INNER)
    mixer_rows = (grouped * group_gain).astype(bf16)
    block_width = INNER // N_TP
    mixer_out = jnp.zeros((BATCH, D), f32)
    for block_index in range(N_TP):
        part_sum = jnp.dot(mixer_rows[:, block_index * block_width:(block_index + 1) * block_width], output_weight[block_index * block_width:(block_index + 1) * block_width], preferred_element_type=f32)
        mixer_out = mixer_out + lax.optimization_barrier(part_sum.astype(bf16)).astype(f32)
    residual = residual + mixer_out
    ffn_rows = rms_scale(residual, channel_gain).astype(bf16)
    dense_hidden = (jax.nn.silu(jnp.dot(ffn_rows, dense_gate, preferred_element_type=f32)) * jnp.dot(ffn_rows, dense_up, preferred_element_type=f32)).astype(bf16)
    dense_out = jnp.dot(dense_hidden, dense_down, preferred_element_type=f32)
    entries = S_DEV * TOPK
    flat_routes = routes.reshape(N_EP, entries)
    onehot = (flat_routes[:, :, None] == jnp.arange(EXPERTS, dtype=jnp.int32)[None, None, :]).astype(jnp.int32)
    rank_before = jnp.cumsum(onehot, axis=1) - onehot
    slot_index = lax.optimization_barrier(jnp.sum(rank_before * onehot, axis=2)).astype(jnp.int32)
    block_rows = ffn_rows.astype(f32).reshape(N_EP, S_DEV, D)
    hidden_width = FF // N_TP

    def one_expert(expert_id):
        chosen = (flat_routes == expert_id)[:, None, :] & (slot_index[:, None, :] == jnp.arange(CAP, dtype=jnp.int32)[None, :, None])
        chosen = lax.optimization_barrier(jnp.sum(chosen.astype(f32).reshape(N_EP, CAP, S_DEV, TOPK), axis=3))
        gathered = jnp.einsum('bcs,bsd->bcd', chosen, block_rows).astype(bf16).reshape(N_EP * CAP, D)
        gate_act = jnp.dot(gathered, expert_gate[expert_id], preferred_element_type=f32)
        up_act = jnp.dot(gathered, expert_up[expert_id], preferred_element_type=f32)
        activated = (jax.nn.silu(gate_act) * up_act).astype(bf16)
        down_whole = expert_down[expert_id]
        total = jnp.zeros((N_EP * CAP, D), f32)
        for block_index in range(N_TP):
            part_sum = jnp.dot(activated[:, block_index * hidden_width:(block_index + 1) * hidden_width], down_whole[block_index * hidden_width:(block_index + 1) * hidden_width], preferred_element_type=f32)
            total = total + lax.optimization_barrier(part_sum.astype(bf16)).astype(f32)
        return total.astype(bf16).reshape(N_EP, CAP, D)
    expert_rows = lax.map(one_expert, jnp.arange(EXPERTS, dtype=jnp.int32))
    block_ids = jnp.broadcast_to(jnp.arange(N_EP, dtype=jnp.int32)[:, None], (N_EP, entries))
    picked = expert_rows[flat_routes, block_ids, slot_index].astype(f32)
    weighted = picked.reshape(N_EP, S_DEV, TOPK, D) * route_weights.reshape(N_EP, S_DEV, TOPK)[..., None]
    expert_out = lax.optimization_barrier(jnp.sum(weighted, axis=2)).reshape(BATCH, D)
    new_tokens = (residual + expert_out + dense_scale * dense_out).astype(bf16)
    return (new_tokens, new_state.reshape(BATCH, HEADS, HEAD_DIM, STATE_DIM), inner_ctx[:, 1:], state_ctx[:, 1:])
```

```python
import functools

import jax
import jax.numpy as jnp
from jax import lax
from jax.experimental import pallas as pl
from jax.experimental.pallas import tpu as pltpu
from jax.sharding import PartitionSpec as P

HEADS = 16
GROUPS = 4
HEAD_DIM = 64
STATE_DIM = 128


eps = 1e-06


def rms_scale(values, norm_gain):
    squares = jnp.mean(values * values, axis=-1, keepdims=True)
    return values * lax.rsqrt(squares + eps) * norm_gain


def silu(v):
    return v / (1.0 + jnp.exp(-v))


def branches(
    ep_size,
    tp_size,
    part,
    tokens,
    gain,
    mix,
    scale,
    gate_hbm,
    up_hbm,
    down_hbm,
    dgate_hbm,
    dup_hbm,
    ddown_hbm,
    out,
    gate_w,
    up_w,
    down_w,
    dgate_w,
    dup_w,
    ddown_w,
    parts,
    mixes,
    residual,
    rows,
    flat,
    packed,
    pre_send,
    pre_recv,
    hidden,
    y_send,
    y_recv,
    z_send,
    z_recv,
    load_sem,
    part_sems,
    mix_sems,
    row_sems,
    relay_sems,
    pre_sems,
    hid_sems,
    y_sems,
    z_sems,
):
    f32 = jnp.float32
    bf16 = jnp.bfloat16
    me_e = lax.axis_index("ep")
    me_t = lax.axis_index("tp")
    half = lax.rem(me_t, 2)
    partner = me_t + 1 - 2 * half
    count, width = part.shape
    half_width = width // 2
    own_width = width // tp_size
    total = ep_size * count
    block = total // tp_size

    def remote(src, dst, sems, slot, to_e, to_t):
        return pltpu.make_async_remote_copy(
            src_ref=src,
            dst_ref=dst,
            send_sem=sems.at[0, slot],
            recv_sem=sems.at[1, slot],
            device_id=(to_e, to_t),
            device_id_type=pl.DeviceIdType.MESH,
        )

    barrier = pltpu.get_barrier_semaphore()
    for d in range(1, ep_size):
        pl.semaphore_signal(
            barrier,
            inc=1,
            device_id=(lax.rem(me_e + d, ep_size), me_t),
            device_id_type=pl.DeviceIdType.MESH,
        )
    for d in range(1, tp_size):
        pl.semaphore_signal(
            barrier,
            inc=1,
            device_id=(me_e, lax.rem(me_t + d, tp_size)),
            device_id_type=pl.DeviceIdType.MESH,
        )
    loads = []
    for i, (src, dst) in enumerate(
        [
            (dgate_hbm, dgate_w),
            (dup_hbm, dup_w),
            (gate_hbm, gate_w),
            (up_hbm, up_w),
            (down_hbm, down_w),
            (ddown_hbm, ddown_w),
        ]
    ):
        copy = pltpu.make_async_copy(src, dst, load_sem.at[i])
        copy.start()
        loads.append(copy)
    pl.semaphore_wait(barrier, ep_size + tp_size - 2)

    ep_peers = [lax.rem(me_e + d, ep_size) for d in range(ep_size)]
    tp_peers = [lax.rem(me_t + d, tp_size) for d in range(tp_size)]
    part_copies = [
        remote(part, parts.at[d], part_sems, d, me_e, tp_peers[d]) for d in range(1, tp_size)
    ]
    for copy in part_copies:
        copy.start()
    mix_copies = [
        remote(mix, mixes.at[d], mix_sems, d, ep_peers[d], me_t) for d in range(1, ep_size)
    ]
    for copy in mix_copies:
        copy.start()

    value = tokens[...].astype(f32) + part[...].astype(f32)
    for d in range(1, tp_size):
        part_copies[d - 1].wait_recv()
        value = value + parts[d].astype(f32)
    residual[...] = value
    ffn = rms_scale(value, gain[...]).astype(bf16)
    rows[0, 0] = ffn[:, :half_width]
    rows[1, 0] = ffn[:, half_width:]
    row_copies = [
        remote(rows.at[half, 0], rows.at[half, d], row_sems, d, ep_peers[d], me_t)
        for d in range(1, ep_size)
    ]
    for copy in row_copies:
        copy.start()
    relay_copies = []
    for d in range(1, ep_size):
        row_copies[d - 1].wait_recv()
        copy = remote(rows.at[half, d], rows.at[half, d], relay_sems, d, me_e, partner)
        copy.start()
        relay_copies.append(copy)
    for copy in relay_copies:
        copy.wait_recv()
    for d in range(ep_size):
        flat[d * count : (d + 1) * count, :half_width] = rows[0, d].astype(f32)
        flat[d * count : (d + 1) * count, half_width:] = rows[1, d].astype(f32)
    packed[...] = flat[...].astype(bf16)

    loads[0].wait()
    loads[1].wait()
    own = pl.ds(pl.multiple_of(me_t * own_width, own_width), own_width)
    for t in range(tp_size):
        piece = packed[t * block : (t + 1) * block, own]
        pre_send[t, 0] = jnp.dot(piece, dgate_w[...], preferred_element_type=f32).astype(bf16)
        pre_send[t, 1] = jnp.dot(piece, dup_w[...], preferred_element_type=f32).astype(bf16)
    pre_copies = [
        remote(pre_send.at[tp_peers[d]], pre_recv.at[d], pre_sems, d, me_e, tp_peers[d])
        for d in range(1, tp_size)
    ]
    for copy in pre_copies:
        copy.start()

    for d in range(1, ep_size):
        mix_copies[d - 1].wait_recv()
    mixes[0] = mix[...]
    loads[2].wait()
    loads[3].wait()
    loads[4].wait()

    chunk_blocks = 8 if ep_size % 8 == 0 else 1
    chunk = chunk_blocks * count

    def experts(step, carry):
        at = pl.ds(pl.multiple_of(step * chunk, chunk), chunk)
        x = packed[at, :]
        gate_act = jnp.dot(x, gate_w[0], preferred_element_type=f32)
        up_act = jnp.dot(x, up_w[0], preferred_element_type=f32)
        activated = (silu(gate_act) * up_act).astype(bf16)
        weights = mixes[pl.ds(step * chunk_blocks, chunk_blocks)].reshape(chunk, mix.shape[1])
        lanes = lax.broadcasted_iota(jnp.int32, weights.shape, 1)
        weight = jnp.sum(jnp.where(lanes == me_e, weights, 0.0), axis=1, keepdims=True)
        for t in range(tp_size):
            y = jnp.dot(
                activated,
                down_w[0, :, t * own_width : (t + 1) * own_width],
                preferred_element_type=f32,
            )
            y_send[t, at, :] = (y * weight).astype(bf16)
        return carry

    lax.fori_loop(0, total // chunk, experts, 0)
    y_copies = [
        remote(y_send.at[tp_peers[d]], y_recv.at[d], y_sems, d, me_e, tp_peers[d])
        for d in range(1, tp_size)
    ]

    gate_sum = pre_send[me_t, 0].astype(f32)
    up_sum = pre_send[me_t, 1].astype(f32)
    for d in range(1, tp_size):
        pre_copies[d - 1].wait_recv()
        gate_sum = gate_sum + pre_recv[d, 0].astype(f32)
        up_sum = up_sum + pre_recv[d, 1].astype(f32)
    hidden[me_t] = (silu(gate_sum) * up_sum).astype(bf16)
    hid_copies = [
        remote(hidden.at[me_t], hidden.at[me_t], hid_sems, d, me_e, tp_peers[d])
        for d in range(1, tp_size)
    ]
    for copy in hid_copies:
        copy.start()
    for copy in y_copies:
        copy.start()
    for d in range(1, tp_size):
        hid_copies[d - 1].wait_recv()
    loads[5].wait()
    for t in range(tp_size):
        dense = jnp.dot(hidden[t], ddown_w[...], preferred_element_type=f32) * scale[...]
        flat[t * block : (t + 1) * block, :own_width] = dense
    for d in range(1, tp_size):
        y_copies[d - 1].wait_recv()

    def combine(step, carry):
        at = pl.ds(pl.multiple_of(step * chunk, chunk), chunk)
        summed = flat[at, :own_width] + y_send[me_t, at, :].astype(f32)
        for d in range(1, tp_size):
            summed = summed + y_recv[d, at, :].astype(f32)
        for i in range(chunk_blocks):
            z_send[step * chunk_blocks + i] = summed[i * count : (i + 1) * count].astype(bf16)
        return carry

    lax.fori_loop(0, total // chunk, combine, 0)
    z_copies = [
        remote(
            z_send.at[d],
            z_recv.at[d],
            z_sems,
            d,
            lax.rem(me_e + ep_size - d, ep_size),
            me_t,
        )
        for d in range(1, ep_size)
    ]
    for copy in z_copies:
        copy.start()
    final = residual[:, own] + z_send[0].astype(f32)
    for d in range(1, ep_size):
        z_copies[d - 1].wait_recv()
        final = final + z_recv[d].astype(f32)
    out[...] = final.astype(bf16)
    for copy in part_copies + mix_copies + row_copies + relay_copies + pre_copies:
        copy.wait_send()
    for copy in hid_copies + y_copies + z_copies:
        copy.wait_send()


def local(
    tokens,
    mixer_gain,
    gate_weight,
    inner_weight,
    state_weight,
    step_weight,
    step_bias,
    decay_log,
    skip_scale,
    inner_kernel,
    state_kernel,
    inner_window,
    state_window,
    recurrent_state,
    group_gain,
    output_weight,
    channel_gain,
    routes,
    route_weights,
    expert_gate,
    expert_up,
    expert_down,
    dense_gate,
    dense_up,
    dense_down,
    dense_scale,
):
    f32 = jnp.float32
    bf16 = jnp.bfloat16
    seq_count = tokens.shape[0]
    residual = tokens.astype(f32)
    normed = rms_scale(residual, mixer_gain).astype(bf16)
    gate_pre = jnp.dot(normed, gate_weight, preferred_element_type=f32)
    inner_pre = jnp.dot(normed, inner_weight, preferred_element_type=f32).astype(bf16)
    state_pre = jnp.stack(
        [
            jnp.dot(normed, state_weight[0], preferred_element_type=f32),
            jnp.dot(normed, state_weight[1], preferred_element_type=f32),
        ],
        axis=1,
    ).astype(bf16)
    step_raw = jnp.dot(normed, step_weight, preferred_element_type=f32)
    inner_ctx = jnp.concatenate([inner_window, inner_pre[:, None, :]], axis=1)
    inner_conv = jax.nn.silu(jnp.sum(inner_ctx.astype(f32) * inner_kernel[None], axis=1))
    state_ctx = jnp.concatenate([state_window, state_pre[:, None]], axis=1)
    state_conv = jax.nn.silu(jnp.sum(state_ctx.astype(f32) * state_kernel[None], axis=1))
    per_group = HEADS // GROUPS
    local_groups = state_conv.shape[-1] // STATE_DIM
    step_size = jax.nn.softplus(step_raw + step_bias)
    decay_rate = jnp.exp(-step_size * jnp.exp(decay_log))
    shaped = (seq_count, local_groups, per_group)
    inner_heads = inner_conv.reshape(seq_count, local_groups, per_group, HEAD_DIM)
    in_vector = state_conv[:, 0].reshape(seq_count, local_groups, STATE_DIM)
    out_vector = state_conv[:, 1].reshape(seq_count, local_groups, STATE_DIM)
    old_state = recurrent_state.reshape(seq_count, local_groups, per_group, HEAD_DIM, STATE_DIM)
    written = (step_size.reshape(shaped)[..., None] * inner_heads)[..., None] * in_vector[
        :, :, None, None, :
    ]
    new_state = old_state * decay_rate.reshape(shaped)[..., None, None] + written
    mixed_out = jnp.sum(new_state * out_vector[:, :, None, None, :], axis=-1)
    mixed_out = (
        mixed_out + skip_scale.reshape(local_groups, per_group)[None, :, :, None] * inner_heads
    )
    gated_out = mixed_out.reshape(seq_count, -1) * jax.nn.silu(gate_pre)
    grouped = rms_scale(gated_out.reshape(seq_count, local_groups, -1), 1.0).reshape(seq_count, -1)
    mixer_rows = (grouped * group_gain).astype(bf16)
    partial_value = jnp.dot(mixer_rows, output_weight, preferred_element_type=f32).astype(bf16)
    ep_size = lax.axis_size("ep")
    tp_size = lax.axis_size("tp")
    width = tokens.shape[1]
    own_width = width // tp_size
    total = ep_size * seq_count
    block = total // tp_size
    hidden_width = dense_gate.shape[1]
    lanes = -(-ep_size // 128) * 128
    mix = jnp.sum(
        jnp.where(
            routes[:, :, None] == jnp.arange(lanes, dtype=jnp.int32)[None, None, :],
            route_weights[:, :, None],
            0.0,
        ),
        axis=1,
    )
    vmem = pl.BlockSpec(memory_space=pltpu.VMEM)
    hbm = pl.BlockSpec(memory_space=pl.ANY)
    dma = pltpu.SemaphoreType.DMA
    new_tokens = pl.pallas_call(
        functools.partial(branches, ep_size, tp_size),
        out_shape=jax.ShapeDtypeStruct((seq_count, own_width), bf16),
        in_specs=[vmem] * 5 + [hbm] * 6,
        out_specs=vmem,
        scratch_shapes=[
            pltpu.VMEM(expert_gate.shape, bf16),
            pltpu.VMEM(expert_up.shape, bf16),
            pltpu.VMEM(expert_down.shape, bf16),
            pltpu.VMEM(dense_gate.shape, bf16),
            pltpu.VMEM(dense_up.shape, bf16),
            pltpu.VMEM(dense_down.shape, bf16),
            pltpu.VMEM((tp_size, seq_count, width), bf16),
            pltpu.VMEM((ep_size, seq_count, lanes), f32),
            pltpu.VMEM((seq_count, width), f32),
            pltpu.VMEM((2, ep_size, seq_count, width // 2), bf16),
            pltpu.VMEM((total, width), f32),
            pltpu.VMEM((total, width), bf16),
            pltpu.VMEM((tp_size, 2, block, hidden_width), bf16),
            pltpu.VMEM((tp_size, 2, block, hidden_width), bf16),
            pltpu.VMEM((tp_size, block, hidden_width), bf16),
            pltpu.VMEM((tp_size, total, own_width), bf16),
            pltpu.VMEM((tp_size, total, own_width), bf16),
            pltpu.VMEM((ep_size, seq_count, own_width), bf16),
            pltpu.VMEM((ep_size, seq_count, own_width), bf16),
            dma((6,)),
            dma((2, tp_size)),
            dma((2, ep_size)),
            dma((2, ep_size)),
            dma((2, ep_size)),
            dma((2, tp_size)),
            dma((2, tp_size)),
            dma((2, tp_size)),
            dma((2, ep_size)),
        ],
        compiler_params=pltpu.CompilerParams(
            collective_id=0, has_side_effects=True, vmem_limit_bytes=60 * 1024 * 1024
        ),
    )(
        partial_value,
        tokens,
        channel_gain[None],
        mix,
        dense_scale[None],
        expert_gate,
        expert_up,
        expert_down,
        dense_gate,
        dense_up,
        dense_down,
    )
    return (
        new_tokens,
        new_state.reshape(seq_count, -1, HEAD_DIM, STATE_DIM),
        inner_ctx[:, 1:],
        state_ctx[:, 1:],
    )


def solution(mesh):
    placed = (
        P("ep", None),
        P(),
        P(None, "tp"),
        P(None, "tp"),
        P(None, None, "tp"),
        P(None, "tp"),
        P("tp"),
        P("tp"),
        P("tp"),
        P(None, "tp"),
        P(None, None, "tp"),
        P("ep", None, "tp"),
        P("ep", None, None, "tp"),
        P("ep", "tp", None, None),
        P("tp"),
        P("tp", None),
        P(),
        P("ep", None),
        P("ep", None),
        P("ep", None, "tp"),
        P("ep", None, "tp"),
        P("ep", "tp", None),
        P("tp", "ep"),
        P("tp", "ep"),
        P("ep", "tp"),
        P("tp"),
    )
    return jax.shard_map(
        local,
        mesh=mesh,
        in_specs=placed,
        out_specs=(
            P("ep", "tp"),
            P("ep", "tp", None, None),
            P("ep", None, "tp"),
            P("ep", None, None, "tp"),
        ),
        check_vma=False,
    )
```

```python
import functools

import jax
import jax.numpy as jnp
from jax import lax
from jax.experimental import pallas as pl
from jax.experimental.pallas import tpu as pltpu
from jax.sharding import PartitionSpec as P

HEADS = 16
GROUPS = 4
HEAD_DIM = 64
STATE_DIM = 128


eps = 1e-06


def rms_scale(values, norm_gain):
    squares = jnp.mean(values * values, axis=-1, keepdims=True)
    return values * lax.rsqrt(squares + eps) * norm_gain


def silu(v):
    return v / (1.0 + jnp.exp(-v))


def dot_rows(rows, columns):
    return lax.dot_general(
        rows, columns, (((1,), (1,)), ((), ())), preferred_element_type=jnp.float32
    )


def branches(
    ep_size,
    tp_size,
    part,
    tokens,
    gain,
    mix,
    scale,
    gate_hbm,
    up_hbm,
    down_hbm,
    dgate_hbm,
    dup_hbm,
    ddown_hbm,
    out,
    gate_w,
    up_w,
    down_w,
    dgate_w,
    dup_w,
    ddown_w,
    parts,
    mixes,
    residual,
    rows,
    flat,
    packed,
    pre_send,
    pre_recv,
    hidden,
    y_send,
    y_recv,
    z_send,
    z_recv,
    load_sem,
    part_sems,
    mix_sems,
    row_sems,
    relay_sems,
    pre_sems,
    hid_sems,
    y_sems,
    z_sems,
):
    f32 = jnp.float32
    bf16 = jnp.bfloat16
    me_e = lax.axis_index("ep")
    me_t = lax.axis_index("tp")
    half = lax.rem(me_t, 2)
    partner = me_t + 1 - 2 * half
    count, width = part.shape
    half_width = width // 2
    own_width = width // tp_size
    total = ep_size * count
    block = total // tp_size

    def remote(src, dst, sems, slot, to_e, to_t):
        return pltpu.make_async_remote_copy(
            src_ref=src,
            dst_ref=dst,
            send_sem=sems.at[0, slot],
            recv_sem=sems.at[1, slot],
            device_id=(to_e, to_t),
            device_id_type=pl.DeviceIdType.MESH,
        )

    barrier = pltpu.get_barrier_semaphore()
    for d in range(1, ep_size):
        pl.semaphore_signal(
            barrier,
            inc=1,
            device_id=(lax.rem(me_e + d, ep_size), me_t),
            device_id_type=pl.DeviceIdType.MESH,
        )
    for d in range(1, tp_size):
        pl.semaphore_signal(
            barrier,
            inc=1,
            device_id=(me_e, lax.rem(me_t + d, tp_size)),
            device_id_type=pl.DeviceIdType.MESH,
        )
    loads = []
    for i, (src, dst) in enumerate(
        [
            (dgate_hbm, dgate_w),
            (dup_hbm, dup_w),
            (gate_hbm, gate_w),
            (up_hbm, up_w),
            (down_hbm, down_w),
            (ddown_hbm, ddown_w),
        ]
    ):
        copy = pltpu.make_async_copy(src, dst, load_sem.at[i])
        copy.start()
        loads.append(copy)
    pl.semaphore_wait(barrier, ep_size + tp_size - 2)

    ep_peers = [lax.rem(me_e + d, ep_size) for d in range(ep_size)]
    tp_peers = [lax.rem(me_t + d, tp_size) for d in range(tp_size)]
    part_copies = [
        remote(part, parts.at[d], part_sems, d, me_e, tp_peers[d]) for d in range(1, tp_size)
    ]
    for copy in part_copies:
        copy.start()
    mix_copies = [
        remote(mix, mixes.at[d], mix_sems, d, ep_peers[d], me_t) for d in range(1, ep_size)
    ]
    for copy in mix_copies:
        copy.start()

    value = tokens[...].astype(f32) + part[...].astype(f32)
    for d in range(1, tp_size):
        part_copies[d - 1].wait_recv()
        value = value + parts[d].astype(f32)
    residual[...] = value
    ffn = rms_scale(value, gain[...]).astype(bf16)
    rows[0, 0] = ffn[:, :half_width]
    rows[1, 0] = ffn[:, half_width:]
    row_copies = [
        remote(rows.at[half, 0], rows.at[half, d], row_sems, d, ep_peers[d], me_t)
        for d in range(1, ep_size)
    ]
    for copy in row_copies:
        copy.start()
    relay_copies = []
    for d in range(1, ep_size):
        row_copies[d - 1].wait_recv()
        copy = remote(rows.at[half, d], rows.at[half, d], relay_sems, d, me_e, partner)
        copy.start()
        relay_copies.append(copy)
    for copy in relay_copies:
        copy.wait_recv()
    for d in range(ep_size):
        flat[d * count : (d + 1) * count, :half_width] = rows[0, d].astype(f32)
        flat[d * count : (d + 1) * count, half_width:] = rows[1, d].astype(f32)
    packed[...] = flat[...].astype(bf16)

    loads[0].wait()
    loads[1].wait()
    own = pl.ds(pl.multiple_of(me_t * own_width, own_width), own_width)
    for t in range(tp_size):
        piece = packed[t * block : (t + 1) * block, own]
        pre_send[t, 0] = dot_rows(piece, dgate_w[...]).astype(bf16)
        pre_send[t, 1] = dot_rows(piece, dup_w[...]).astype(bf16)
    pre_copies = [
        remote(pre_send.at[tp_peers[d]], pre_recv.at[d], pre_sems, d, me_e, tp_peers[d])
        for d in range(1, tp_size)
    ]
    for copy in pre_copies:
        copy.start()

    for d in range(1, ep_size):
        mix_copies[d - 1].wait_recv()
    mixes[0] = mix[...]
    loads[2].wait()
    loads[3].wait()
    loads[4].wait()

    chunk_blocks = 8 if ep_size % 8 == 0 else 1
    chunk = chunk_blocks * count

    def experts(step, carry):
        at = pl.ds(pl.multiple_of(step * chunk, chunk), chunk)
        x = packed[at, :]
        gate_act = dot_rows(x, gate_w[0])
        up_act = dot_rows(x, up_w[0])
        activated = (silu(gate_act) * up_act).astype(bf16)
        weights = mixes[pl.ds(step * chunk_blocks, chunk_blocks)].reshape(chunk, mix.shape[1])
        lanes = lax.broadcasted_iota(jnp.int32, weights.shape, 1)
        weight = jnp.sum(jnp.where(lanes == me_e, weights, 0.0), axis=1, keepdims=True)
        for t in range(tp_size):
            y = jnp.dot(
                activated,
                down_w[0, :, t * own_width : (t + 1) * own_width],
                preferred_element_type=f32,
            )
            y_send[t, at, :] = (y * weight).astype(bf16)
        return carry

    lax.fori_loop(0, total // chunk, experts, 0)
    y_copies = [
        remote(y_send.at[tp_peers[d]], y_recv.at[d], y_sems, d, me_e, tp_peers[d])
        for d in range(1, tp_size)
    ]

    gate_sum = pre_send[me_t, 0].astype(f32)
    up_sum = pre_send[me_t, 1].astype(f32)
    for d in range(1, tp_size):
        pre_copies[d - 1].wait_recv()
        gate_sum = gate_sum + pre_recv[d, 0].astype(f32)
        up_sum = up_sum + pre_recv[d, 1].astype(f32)
    hidden[me_t] = (silu(gate_sum) * up_sum).astype(bf16)
    hid_copies = [
        remote(hidden.at[me_t], hidden.at[me_t], hid_sems, d, me_e, tp_peers[d])
        for d in range(1, tp_size)
    ]
    for copy in hid_copies:
        copy.start()
    for copy in y_copies:
        copy.start()
    for d in range(1, tp_size):
        hid_copies[d - 1].wait_recv()
    loads[5].wait()
    for t in range(tp_size):
        dense = jnp.dot(hidden[t], ddown_w[...], preferred_element_type=f32) * scale[...]
        flat[t * block : (t + 1) * block, :own_width] = dense
    for d in range(1, tp_size):
        y_copies[d - 1].wait_recv()

    def combine(step, carry):
        at = pl.ds(pl.multiple_of(step * chunk, chunk), chunk)
        summed = flat[at, :own_width] + y_send[me_t, at, :].astype(f32)
        for d in range(1, tp_size):
            summed = summed + y_recv[d, at, :].astype(f32)
        for i in range(chunk_blocks):
            z_send[step * chunk_blocks + i] = summed[i * count : (i + 1) * count].astype(bf16)
        return carry

    lax.fori_loop(0, total // chunk, combine, 0)
    z_copies = [
        remote(
            z_send.at[d],
            z_recv.at[d],
            z_sems,
            d,
            lax.rem(me_e + ep_size - d, ep_size),
            me_t,
        )
        for d in range(1, ep_size)
    ]
    for copy in z_copies:
        copy.start()
    final = residual[:, own] + z_send[0].astype(f32)
    for d in range(1, ep_size):
        z_copies[d - 1].wait_recv()
        final = final + z_recv[d].astype(f32)
    out[...] = final.astype(bf16)
    for copy in part_copies + mix_copies + row_copies + relay_copies + pre_copies:
        copy.wait_send()
    for copy in hid_copies + y_copies + z_copies:
        copy.wait_send()


def local(
    tokens,
    mixer_gain,
    gate_weight,
    inner_weight,
    state_weight,
    step_weight,
    step_bias,
    decay_log,
    skip_scale,
    inner_kernel,
    state_kernel,
    inner_window,
    state_window,
    recurrent_state,
    group_gain,
    output_weight,
    channel_gain,
    routes,
    route_weights,
    expert_gate,
    expert_up,
    expert_down,
    dense_gate,
    dense_up,
    dense_down,
    dense_scale,
):
    f32 = jnp.float32
    bf16 = jnp.bfloat16
    seq_count = tokens.shape[0]
    residual = tokens.astype(f32)
    normed = rms_scale(residual, mixer_gain).astype(bf16)
    gate_pre = jnp.dot(normed, gate_weight, preferred_element_type=f32)
    inner_pre = jnp.dot(normed, inner_weight, preferred_element_type=f32).astype(bf16)
    state_pre = jnp.stack(
        [
            jnp.dot(normed, state_weight[0], preferred_element_type=f32),
            jnp.dot(normed, state_weight[1], preferred_element_type=f32),
        ],
        axis=1,
    ).astype(bf16)
    step_raw = jnp.dot(normed, step_weight, preferred_element_type=f32)
    inner_ctx = jnp.concatenate([inner_window, inner_pre[:, None, :]], axis=1)
    inner_conv = jax.nn.silu(jnp.sum(inner_ctx.astype(f32) * inner_kernel[None], axis=1))
    state_ctx = jnp.concatenate([state_window, state_pre[:, None]], axis=1)
    state_conv = jax.nn.silu(jnp.sum(state_ctx.astype(f32) * state_kernel[None], axis=1))
    per_group = HEADS // GROUPS
    local_groups = state_conv.shape[-1] // STATE_DIM
    step_size = jax.nn.softplus(step_raw + step_bias)
    decay_rate = jnp.exp(-step_size * jnp.exp(decay_log))
    shaped = (seq_count, local_groups, per_group)
    inner_heads = inner_conv.reshape(seq_count, local_groups, per_group, HEAD_DIM)
    in_vector = state_conv[:, 0].reshape(seq_count, local_groups, STATE_DIM)
    out_vector = state_conv[:, 1].reshape(seq_count, local_groups, STATE_DIM)
    old_state = recurrent_state.reshape(seq_count, local_groups, per_group, HEAD_DIM, STATE_DIM)
    written = (step_size.reshape(shaped)[..., None] * inner_heads)[..., None] * in_vector[
        :, :, None, None, :
    ]
    new_state = old_state * decay_rate.reshape(shaped)[..., None, None] + written
    mixed_out = jnp.sum(new_state * out_vector[:, :, None, None, :], axis=-1)
    mixed_out = (
        mixed_out + skip_scale.reshape(local_groups, per_group)[None, :, :, None] * inner_heads
    )
    gated_out = mixed_out.reshape(seq_count, -1) * jax.nn.silu(gate_pre)
    grouped = rms_scale(gated_out.reshape(seq_count, local_groups, -1), 1.0).reshape(seq_count, -1)
    mixer_rows = (grouped * group_gain).astype(bf16)
    partial_value = jnp.dot(mixer_rows, output_weight, preferred_element_type=f32).astype(bf16)
    ep_size = lax.axis_size("ep")
    tp_size = lax.axis_size("tp")
    width = tokens.shape[1]
    own_width = width // tp_size
    total = ep_size * seq_count
    block = total // tp_size
    hidden_width = dense_gate.shape[1]
    expert_gate = jnp.swapaxes(expert_gate, 1, 2)
    expert_up = jnp.swapaxes(expert_up, 1, 2)
    dense_gate = dense_gate.T
    dense_up = dense_up.T
    lanes = -(-ep_size // 128) * 128
    mix = jnp.sum(
        jnp.where(
            routes[:, :, None] == jnp.arange(lanes, dtype=jnp.int32)[None, None, :],
            route_weights[:, :, None],
            0.0,
        ),
        axis=1,
    )
    vmem = pl.BlockSpec(memory_space=pltpu.VMEM)
    hbm = pl.BlockSpec(memory_space=pl.ANY)
    dma = pltpu.SemaphoreType.DMA
    new_tokens = pl.pallas_call(
        functools.partial(branches, ep_size, tp_size),
        out_shape=jax.ShapeDtypeStruct((seq_count, own_width), bf16),
        in_specs=[vmem] * 5 + [hbm] * 6,
        out_specs=vmem,
        scratch_shapes=[
            pltpu.VMEM(expert_gate.shape, bf16),
            pltpu.VMEM(expert_up.shape, bf16),
            pltpu.VMEM(expert_down.shape, bf16),
            pltpu.VMEM(dense_gate.shape, bf16),
            pltpu.VMEM(dense_up.shape, bf16),
            pltpu.VMEM(dense_down.shape, bf16),
            pltpu.VMEM((tp_size, seq_count, width), bf16),
            pltpu.VMEM((ep_size, seq_count, lanes), f32),
            pltpu.VMEM((seq_count, width), f32),
            pltpu.VMEM((2, ep_size, seq_count, width // 2), bf16),
            pltpu.VMEM((total, width), f32),
            pltpu.VMEM((total, width), bf16),
            pltpu.VMEM((tp_size, 2, block, hidden_width), bf16),
            pltpu.VMEM((tp_size, 2, block, hidden_width), bf16),
            pltpu.VMEM((tp_size, block, hidden_width), bf16),
            pltpu.VMEM((tp_size, total, own_width), bf16),
            pltpu.VMEM((tp_size, total, own_width), bf16),
            pltpu.VMEM((ep_size, seq_count, own_width), bf16),
            pltpu.VMEM((ep_size, seq_count, own_width), bf16),
            dma((6,)),
            dma((2, tp_size)),
            dma((2, ep_size)),
            dma((2, ep_size)),
            dma((2, ep_size)),
            dma((2, tp_size)),
            dma((2, tp_size)),
            dma((2, tp_size)),
            dma((2, ep_size)),
        ],
        compiler_params=pltpu.CompilerParams(
            collective_id=0, has_side_effects=True, vmem_limit_bytes=60 * 1024 * 1024
        ),
    )(
        partial_value,
        tokens,
        channel_gain[None],
        mix,
        dense_scale[None],
        expert_gate,
        expert_up,
        expert_down,
        dense_gate,
        dense_up,
        dense_down,
    )
    return (
        new_tokens,
        new_state.reshape(seq_count, -1, HEAD_DIM, STATE_DIM),
        inner_ctx[:, 1:],
        state_ctx[:, 1:],
    )


def solution(mesh):
    placed = (
        P("ep", None),
        P(),
        P(None, "tp"),
        P(None, "tp"),
        P(None, None, "tp"),
        P(None, "tp"),
        P("tp"),
        P("tp"),
        P("tp"),
        P(None, "tp"),
        P(None, None, "tp"),
        P("ep", None, "tp"),
        P("ep", None, None, "tp"),
        P("ep", "tp", None, None),
        P("tp"),
        P("tp", None),
        P(),
        P("ep", None),
        P("ep", None),
        P("ep", None, "tp"),
        P("ep", None, "tp"),
        P("ep", "tp", None),
        P("tp", "ep"),
        P("tp", "ep"),
        P("ep", "tp"),
        P("tp"),
    )
    return jax.shard_map(
        local,
        mesh=mesh,
        in_specs=placed,
        out_specs=(
            P("ep", "tp"),
            P("ep", "tp", None, None),
            P("ep", None, "tp"),
            P("ep", None, None, "tp"),
        ),
        check_vma=False,
    )
```
